32 devices in a mesh: sp: 8 (over z, x), tp: 4 (over y, core).
Axes of the slice: x: 2, y: 2, z: 4, core: 2. Of those that a mesh axis runs over, the one named last changes fastest.
Arguments:
- residual: bfloat16 [3072, 2048], P(('sp', 'tp')), may hold values from -6 to 6
- queries: bfloat16 [3072, 1024], P('sp', 'tp'), may hold values from -2.5 to 2.5
- keys: bfloat16 [3072, 256], P('sp', 'tp'), may hold values from -2.5 to 2.5
- values: bfloat16 [3072, 256], P('sp', 'tp'), may hold values from -6 to 6
- documents: int32 [3072], P('sp'), may hold values from 0 to 4, never falling along the last dimension, each value on 1 to 1536 neighbouring positions
- sink: float32 [16], P('tp'), may hold values from 3 to 7
- out_weight: bfloat16 [1024, 2048], replicated, may hold values from -0.1875 to 0.1875
- mix_gain: float32 [2048], replicated, may hold values from 0.1 to 1.9
- ffn_gain: float32 [2048], replicated, may hold values from 0.1 to 1.9
- out_gain: float32 [2048], replicated, may hold values from 0.1 to 1.9
- routes: int32 [3072, 4], P(('sp', 'tp')), may hold values from 0 to 7, all different within a row; in each aligned block of 96 rows (0 to 95, 96 to 191, ...) at most 64 rows name the same one
- route_logits: float32 [3072, 4], P(('sp', 'tp')), may hold values from -4 to 4
- gate_weight: bfloat16 [8, 2048, 2048], P('sp', None, 'tp'), may hold values from -1.41421356 to 1.41421356
- up_weight: bfloat16 [8, 2048, 2048], P('sp', None, 'tp'), may hold values from -1.41421356 to 1.41421356
- down_weight: bfloat16 [8, 2048, 2048], P('sp', 'tp'), may hold values from -0.125 to 0.125
Outputs:
- mixed: bfloat16 [3072, 2048], P(('sp', 'tp'))
The draws below stay inside these ranges and needn't reach their ends.
Inputs may be any that keep to these rules, and one draw needn't show every extreme that they name: `routes`: each row names 4 different experts. In each aligned block of rows held by one device, no expert is named by more than 64 rows, a bound that some block reaches. `documents`: document numbers never fall along the positions; each document has 1 to 1536 positions, and one has exactly 1536.
All inputs are finite; a program needn't handle non-finite values.
Results may differ from the reference program's by a relative error of at most 0.017.
Values may be sent and summed in bfloat16 or wider, within the bound.
No kernel may reach another device: no remote copies, remote signals or barrier semaphores. Data moves between devices by JAX's collectives and lax.ppermute only.
A program may use at most 128 MiB of HBM per device.

```python
import math
import jax
import jax.numpy as jnp
import numpy as np
from jax import lax

D = 2048
QH = 16
KVH = 4
HD = 64
FF = 2048
TOPK = 4
W = 128
TOK_DEV = 384
TOKENS = 3072
EXPERTS = 8
CAP = 64
DOCS = 5
DOC_MOST = 1536
N_TP = 4


def column_scaled(key):
    base_key, scale_key = jax.random.split(key)
    shape = (EXPERTS, D, FF)
    base = jnp.clip(jax.random.normal(base_key, shape, jnp.float32), -4.0, 4.0)
    column_scale = jnp.exp(jax.random.uniform(scale_key, (EXPERTS, 1, FF), jnp.float32, 0.0, 2.3025851))
    return (base * column_scale * D ** (-0.5)).astype(jnp.bfloat16)


def draw_gate_weight(key, part):
    return column_scaled(jax.random.fold_in(key, 11))


def draw_up_weight(key, part):
    return column_scaled(jax.random.fold_in(key, 23))


def block_scale(own_key, dims, cuts, smallest, high):
    factor_of, own = 1.0, jax.random.fold_in(own_key, 6)
    for dim, parts in cuts:
        heights = jnp.exp(jax.random.uniform(jax.random.fold_in(own, dim), (parts,), jnp.float32, smallest / len(cuts), high / len(cuts)))
        factor_of = factor_of * jnp.repeat(heights, dims[dim] // parts).reshape([-1 if axis == dim else 1 for axis in range(len(dims))])
    return factor_of


def profile(count, total, limit, skew):
    weights = [(1 << 20) // math.isqrt(grade ** skew) + 1 for grade in range(2, count + 1)]
    rest, given = total - limit - (count - 1), [1] * (count - 1)
    while rest > 0:
        free = [i for i in range(count - 1) if given[i] < limit]
        mass, remaining = sum([weights[i] for i in free]), rest
        for i in free:
            addition = min(limit - given[i], max(1, remaining * weights[i] // mass), rest)
            given[i] = given[i] + addition
            rest = rest - addition
    return np.array([limit] + given)


def uneven(own_key, amount, total, limit, skew):
    if amount == 2:
        one = jax.random.randint(own_key, (), max(1, total - limit), min(limit, total - 1) + 1)
        return jnp.stack([one, total - one])
    tallies = jnp.asarray(profile(amount, total, limit, skew), jnp.int32)
    couples = (amount - 1) // 2
    giver, taker = tallies[1:1 + 2 * couples:2], tallies[2:2 + 2 * couples:2]
    margin = jnp.minimum(giver - 1, limit - taker)
    shifted = jax.random.randint(jax.random.fold_in(own_key, 1), (couples,), 0, 1 << 20) % (margin + 1)
    tallies = tallies.at[1:1 + 2 * couples:2].set(giver - shifted).at[2:2 + 2 * couples:2].set(taker + shifted)
    return tallies[jax.random.permutation(jax.random.fold_in(own_key, 2), amount)]


def deal_out(stream_key, own, number, rows, count, top, bound, skew):
    sequence = jax.random.permutation(stream_key, count)
    packed, common = load_shares(count, rows * top, bound, skew, True), load_shares(count, rows * top, bound, skew, False)
    places = jnp.arange(count)

    def named(tallies, turn):
        used = int((tallies > 0).sum())
        fixed = max(1, used // 4)
        moved = fixed + (places - fixed + turn * (used - fixed)) % max(1, count - fixed)
        return jnp.zeros((count,), jnp.int32).at[sequence[jnp.where(places < fixed, places, moved)]].set(jnp.asarray(tallies, jnp.int32))

    tallies = jnp.where(number % 4 == 0, named(packed, number // 4), named(common, number - number // 4 - 1))
    mixed = jax.random.permutation(jax.random.fold_in(own, 3), count)
    giver, taker = mixed[0:count // 2 * 2:2], mixed[1:count // 2 * 2:2]
    slack = jnp.minimum(tallies[giver] - 1, bound - tallies[taker]) // 2
    slack = jnp.where((giver == sequence[0]) | (taker == sequence[0]) | (tallies[taker] == 0), 0, jnp.maximum(slack, 0))
    moved = jax.random.randint(jax.random.fold_in(own, 4), (count // 2,), 0, 1 << 20) % (slack + 1)
    tallies = tallies.at[giver].add(-moved).at[taker].add(moved)
    members = jnp.searchsorted(jnp.cumsum(tallies), jnp.arange(rows * top), side="right").astype(jnp.int32)
    listing = members.reshape(top, rows).T
    listing = listing[jax.random.permutation(jax.random.fold_in(own, 1), rows)]
    turn = jax.random.randint(jax.random.fold_in(own, 2), (rows, 1), 0, top)
    return jnp.take_along_axis(listing, (jnp.arange(top)[None, :] + turn) % top, axis=1)


def load_shares(number_of, total, limit, skew, full):
    weights = [(1 << 20) // math.isqrt(rank ** skew) + 1 for rank in range(1, number_of + 1)]
    largest = limit if full else min(limit, max(-(-total // number_of), total * weights[0] // sum(weights)))
    least = 1 if total - largest >= number_of - 1 else 0
    given, rest = [largest] + [least] * (number_of - 1), total - largest - least * (number_of - 1)
    while rest > 0:
        candidates = [i for i in range(1, number_of) if given[i] < largest] or [i for i in range(1, number_of) if given[i] < limit]
        mass, budget = sum([weights[i] for i in candidates]), rest
        for i in candidates:
            more = min(limit - given[i], max(1, budget * weights[i] // mass), rest)
            given[i] = given[i] + more
            rest = rest - more
    return np.array(given)


def noise(key, shape, width, most, shards=(), kind=jnp.bfloat16):
    array = jax.random.normal(key, shape, jnp.float32) * width
    if len(shards) > 0:
        array = block_scale(key, shape, shards, -0.22, 0.18) * array
    return jnp.clip(array, min=-most, max=most).astype(kind)


def setup_inputs(seed: int = 0) -> dict:
    splits = jax.random.split(jax.random.key(seed), 16)
    residual = noise(splits[0], (TOKENS, D), 1.0, 6.0, ((0, 32),))
    queries = noise(splits[1], (TOKENS, QH * HD), 1.0, 2.5, ((0, 8), (1, 4)))
    keys = noise(splits[2], (TOKENS, KVH * HD), 1.0, 2.5, ((0, 8), (1, 4)))
    values = noise(splits[3], (TOKENS, KVH * HD), 1.0, 6.0, ((0, 8), (1, 4)))
    documents = jnp.searchsorted(jnp.cumsum(uneven(splits[4], DOCS, TOKENS, DOC_MOST, 1)), jnp.arange(TOKENS), side="right").astype(jnp.int32)
    sink = jnp.clip(3.0 + 4.0 * jax.random.uniform(splits[5], (QH,), jnp.float32) ** block_scale(splits[5], (QH,), ((0, 4),), -0.2, 0.2), 3.0, 7.0)
    out_weight = noise(splits[6], (QH * HD, D), (QH * HD) ** -0.5, 0.1875)
    mix_gain = jnp.clip(1.0 + 0.18 * jax.random.normal(splits[7], (D,), jnp.float32), 0.1, 1.9)
    ffn_gain = jnp.clip(1.0 + 0.18 * jax.random.normal(splits[8], (D,), jnp.float32), 0.1, 1.9)
    out_gain = jnp.clip(1.0 + 0.18 * jax.random.normal(splits[9], (D,), jnp.float32), 0.1, 1.9)
    routes_keys = jax.random.split(jax.random.fold_in(splits[10], 1), TOKENS // (TOK_DEV // N_TP))
    routes_turns = jax.random.permutation(jax.random.fold_in(splits[10], 3), TOKENS // (TOK_DEV // N_TP))
    routes = jax.vmap(lambda own, number: deal_out(jax.random.fold_in(splits[10], 2), own, number, TOK_DEV // N_TP, EXPERTS, TOPK, CAP, 2))(routes_keys, routes_turns).reshape((TOKENS, TOPK))
    route_logits = noise(splits[11], (TOKENS, TOPK), 1.0, 4.0, ((0, 32),), jnp.float32)
    gate_weight = draw_gate_weight(jax.random.fold_in(splits[15], 71), 0)
    up_weight = draw_up_weight(jax.random.fold_in(splits[15], 71), 0)
    down_weight = noise(splits[14], (EXPERTS, FF, D), FF ** -0.5, 0.125, ((0, 8), (1, 4)))
    return {"residual": residual, "queries": queries, "keys": keys, "values": values, "documents": documents, "sink": sink, "out_weight": out_weight, "mix_gain": mix_gain, "ffn_gain": ffn_gain, "out_gain": out_gain, "routes": routes, "route_logits": route_logits, "gate_weight": gate_weight, "up_weight": up_weight, "down_weight": down_weight}


def turn_heads(block, positions, head_count):
    total = block.shape[0]
    heads = block.astype(jnp.float32).reshape(total, head_count, HD)
    half_size = HD // 2
    inverse = 10000.0 ** (-jnp.arange(half_size, dtype=jnp.float32) / half_size)
    angles = positions.astype(jnp.float32)[:, None] * inverse[None, :]
    cosine = jnp.cos(angles)[:, None, :]
    sine = jnp.sin(angles)[:, None, :]
    first_half = heads[..., :half_size]
    second_half = heads[..., half_size:]
    turned = jnp.concatenate([first_half * cosine - second_half * sine, second_half * cosine + first_half * sine], axis=-1)
    return turned.reshape(total, head_count * HD).astype(jnp.bfloat16)

def rms_scale(vector):
    return vector * lax.rsqrt(lax.optimization_barrier(jnp.mean(vector * vector, axis=-1, keepdims=True)) + 1e-06)

def windows(padded_rows, blocks):
    tiled = padded_rows.reshape((blocks + 2, W) + padded_rows.shape[1:])
    return jnp.concatenate([tiled[:-2], tiled[1:-1], tiled[2:]], axis=1)

def reference(residual, queries, keys, values, documents, sink, out_weight, mix_gain, ffn_gain, out_gain, routes, route_logits, gate_weight, up_weight, down_weight):
    total = TOKENS
    group_size = QH // KVH
    positions = jnp.arange(total, dtype=jnp.int32)
    q_turned = turn_heads(queries, positions, QH)
    k_turned = turn_heads(keys, positions, KVH)
    blocks = total // W
    query_blocks = q_turned.reshape(blocks, W, KVH, group_size, HD)
    key_pad = jnp.pad(k_turned.reshape(total, KVH, HD), ((W, W), (0, 0), (0, 0)))
    value_pad = jnp.pad(values.reshape(total, KVH, HD), ((W, W), (0, 0), (0, 0)))
    doc_pad = jnp.pad(documents, (W, W), constant_values=-1)
    key_win = windows(key_pad, blocks)
    value_win = windows(value_pad, blocks)
    doc_win = windows(doc_pad, blocks)
    doc_query = documents.reshape(blocks, W)
    block_ids = jnp.arange(blocks, dtype=jnp.int32)[:, None, None]
    query_pos = block_ids * W + jnp.arange(W, dtype=jnp.int32)[None, :, None]
    key_pos = (block_ids - 1) * W + jnp.arange(3 * W, dtype=jnp.int32)[None, None, :]
    keep_mask = (jnp.abs(query_pos - key_pos) <= W) & (key_pos >= 0) & (key_pos < total)
    keep_mask = keep_mask & (doc_query[:, :, None] == doc_win[:, None, :])
    sink_terms = jnp.exp(sink).reshape(KVH, group_size, 1, 1)

    def one_block(operands):
        query_one, key_one, value_one, mask_one = operands
        scores = jnp.einsum('qhgd,khd->hgqk', query_one.astype(jnp.float32), key_one.astype(jnp.float32)) * HD ** (-0.5)
        exponent = jnp.where(mask_one[None, None], jnp.exp(scores), 0.0)
        denominator = lax.optimization_barrier(jnp.sum(exponent, axis=-1, keepdims=True)) + sink_terms
        probs = (exponent / denominator).astype(jnp.bfloat16)
        attended_one = jnp.einsum('hgqk,khd->qhgd', probs.astype(jnp.float32), value_one.astype(jnp.float32))
        return attended_one.astype(jnp.bfloat16).reshape(W, QH * HD)
    attended = lax.map(one_block, (query_blocks, key_win, value_win, keep_mask)).reshape(total, QH * HD)
    projected = jnp.dot(attended, out_weight, preferred_element_type=jnp.float32)
    after_mix = residual.astype(jnp.float32) + rms_scale(projected) * mix_gain
    normed = (rms_scale(after_mix) * ffn_gain).astype(jnp.bfloat16)
    row_block = 128
    assigned = total * TOPK
    flat_routes = routes.reshape(assigned).astype(jnp.int32)
    order = jnp.argsort(flat_routes, stable=True).astype(jnp.int32)
    sorted_experts = flat_routes[order]
    sorted_tokens = (order // TOPK).astype(jnp.int32)
    counts = lax.optimization_barrier(jnp.sum((flat_routes[:, None] == jnp.arange(EXPERTS, dtype=jnp.int32)[None, :]).astype(jnp.int32), axis=0))
    padded_counts = (counts + row_block - 1) // row_block * row_block
    starts = jnp.cumsum(counts) - counts
    padded_ends = jnp.cumsum(padded_counts)
    padded_starts = padded_ends - padded_counts
    slot_rows = (padded_starts[sorted_experts] + jnp.arange(assigned, dtype=jnp.int32) - starts[sorted_experts]).astype(jnp.int32)
    block_count = -(-(assigned + EXPERTS * (row_block - 1)) // row_block)
    padded_total = block_count * row_block
    row_token = jnp.full((padded_total,), total, dtype=jnp.int32).at[slot_rows].set(sorted_tokens)
    with_zero = jnp.concatenate([normed, jnp.zeros((1, D), jnp.bfloat16)], axis=0)
    expert_rows = with_zero[row_token].reshape(block_count, row_block, D)
    block_expert = jnp.minimum(jnp.searchsorted(padded_ends, jnp.arange(block_count, dtype=jnp.int32) * row_block, side='right'), EXPERTS - 1).astype(jnp.int32)
    quarter = FF // N_TP

    def expert_block(operands):
        rows_in, expert_id = operands
        gate_pre = jnp.dot(rows_in, gate_weight[expert_id], preferred_element_type=jnp.float32)
        up_pre = jnp.dot(rows_in, up_weight[expert_id], preferred_element_type=jnp.float32)
        gated = jnp.minimum(gate_pre, 7.0)
        upper = jnp.clip(up_pre, -7.0, 7.0)
        hidden = ((upper + 1.0) * gated * jax.nn.sigmoid(1.702 * gated)).astype(jnp.bfloat16)
        down_one = down_weight[expert_id]
        summed = jnp.zeros((rows_in.shape[0], D), jnp.float32)
        for source in range(N_TP):
            partial_out = jnp.dot(hidden[:, source * quarter:(source + 1) * quarter], down_one[source * quarter:(source + 1) * quarter], preferred_element_type=jnp.float32)
            summed = summed + lax.optimization_barrier(partial_out.astype(jnp.bfloat16)).astype(jnp.float32)
        return summed.astype(jnp.bfloat16)
    expert_out = lax.map(expert_block, (expert_rows, block_expert)).reshape(padded_total, D)
    row_of = jnp.zeros((assigned,), jnp.int32).at[order].set(slot_rows).reshape(total, TOPK)
    exp_logits = jnp.exp(route_logits)
    route_weights = exp_logits / lax.optimization_barrier(jnp.sum(exp_logits, axis=-1, keepdims=True))
    expert_mix = jnp.zeros((total, D), jnp.float32)
    for choice_index in range(TOPK):
        expert_mix = expert_mix + route_weights[:, choice_index:choice_index + 1] * expert_out[row_of[:, choice_index]].astype(jnp.float32)
    return (after_mix + rms_scale(expert_mix) * out_gain).astype(jnp.bfloat16)
```

```python
import functools

import jax
import jax.numpy as jnp
from jax import lax
from jax.sharding import Mesh
from jax.sharding import PartitionSpec as P


HD = 64
TOPK = 4
W = 128


def extended(block, sides, width):
    for axis, dim in sides:
        count = lax.axis_size(axis)
        forward = [(i, i + 1) for i in range(count - 1)]
        backward = [(target, source) for source, target in forward]
        low = lax.ppermute(
            lax.slice_in_dim(block, block.shape[dim] - width, None, axis=dim), axis, forward
        )
        high = lax.ppermute(lax.slice_in_dim(block, 0, width, axis=dim), axis, backward)
        block = jnp.concatenate([low, block, high], axis=dim)
    return block


def turn_heads(block, positions, head_count):
    total = block.shape[0]
    heads = block.astype(jnp.float32).reshape(total, head_count, HD)
    half_size = HD // 2
    inverse = 10000.0 ** (-jnp.arange(half_size, dtype=jnp.float32) / half_size)
    angles = positions.astype(jnp.float32)[:, None] * inverse[None, :]
    cosine = jnp.cos(angles)[:, None, :]
    sine = jnp.sin(angles)[:, None, :]
    first_half = heads[..., :half_size]
    second_half = heads[..., half_size:]
    turned = jnp.concatenate(
        [first_half * cosine - second_half * sine, second_half * cosine + first_half * sine],
        axis=-1,
    )
    return turned.reshape(total, head_count * HD).astype(jnp.bfloat16)


def rms_scale(vector):
    return vector * lax.rsqrt(jnp.mean(vector * vector, axis=-1, keepdims=True) + 1e-06)


def windows(padded_rows, blocks):
    tiled = padded_rows.reshape((blocks + 2, W) + padded_rows.shape[1:])
    return jnp.concatenate([tiled[:-2], tiled[1:-1], tiled[2:]], axis=1)


def assign_slots(route_rows, expert_count, capacity):
    flat_routes = route_rows.reshape(route_rows.shape[0] * TOPK)
    onehot_hits = (
        flat_routes[:, None] == jnp.arange(expert_count, dtype=jnp.int32)[None, :]
    ).astype(jnp.int32)
    slot_number = jnp.sum(jnp.cumsum(onehot_hits, axis=0) * onehot_hits, axis=1) - 1
    return flat_routes * capacity + slot_number


def routed_experts(sp, tp, normed, routes, route_weights, gate_weight, up_weight, down_weight):
    own_rows = normed.shape[0]
    sp_count = lax.axis_size(sp)
    local_experts = gate_weight.shape[0]
    expert_count = local_experts * sp_count
    capacity = max(2, own_rows * TOPK * 4 // (3 * expert_count))
    slot_index = assign_slots(routes, expert_count, capacity)
    token_of = jnp.arange(own_rows * TOPK, dtype=jnp.int32) // TOPK
    model_width = normed.shape[1]
    filled = jnp.full((expert_count * capacity,), own_rows, jnp.int32).at[slot_index].set(token_of)
    with_zero = jnp.concatenate([normed, jnp.zeros((1, model_width), jnp.bfloat16)], axis=0)
    outgoing = with_zero[filled].reshape(expert_count, capacity, model_width)
    incoming = lax.all_to_all(outgoing, sp, split_axis=0, concat_axis=1, tiled=True)
    rows_in = lax.all_gather(incoming, tp, axis=1, tiled=True)
    gate_pre = jnp.einsum("erd,edf->erf", rows_in, gate_weight, preferred_element_type=jnp.float32)
    up_pre = jnp.einsum("erd,edf->erf", rows_in, up_weight, preferred_element_type=jnp.float32)
    gated = jnp.minimum(gate_pre, 7.0)
    upper = jnp.clip(up_pre, -7.0, 7.0)
    hidden = ((upper + 1.0) * gated * jax.nn.sigmoid(1.702 * gated)).astype(jnp.bfloat16)
    terms = jnp.einsum("erf,efd->erd", hidden, down_weight, preferred_element_type=jnp.float32)
    own_terms = lax.psum_scatter(terms.astype(jnp.bfloat16), tp, scatter_dimension=1, tiled=True)
    returned = lax.all_to_all(own_terms, sp, split_axis=1, concat_axis=0, tiled=True)
    picked = returned.reshape(expert_count * capacity, model_width)[slot_index]
    picked = picked.reshape(own_rows, TOPK, model_width).astype(jnp.float32)
    return jnp.einsum("rk,rkd->rd", route_weights, picked)


def shift(block, axis, step):
    count = lax.axis_size(axis)
    return lax.ppermute(block, axis, [(i, (i + step) % count) for i in range(count)])


def dense_experts(normed, routes, route_weights, weights, peer_weights):
    nz, nx, ny = lax.axis_size("sz"), lax.axis_size("sx"), lax.axis_size("ty")
    iz, ix, iy = lax.axis_index("sz"), lax.axis_index("sx"), lax.axis_index("ty")
    half = normed.shape[0] // 2
    named = routes[:, :, None] == jnp.arange(nz * nx, dtype=jnp.int32)
    table = jnp.sum(jnp.where(named, route_weights[:, :, None], 0.0), axis=1).T
    tables = lax.all_gather(table, ("sz", "sx", "ty"), axis=0, tiled=False)
    tables = lax.dynamic_index_in_dim(tables, iz * nx + ix, axis=1, keepdims=False)

    def cross_x(block):
        return shift(block, "sx", 1)

    def cross_y(block):
        return block if ny == 1 else shift(block, "ty", 1)

    blocks = [normed] + [shift(normed, "sz", step) for step in range(1, nz)]
    own_a = jnp.concatenate([block[:half] for block in blocks], axis=0)
    own_b = jnp.concatenate([block[half:] for block in blocks], axis=0)
    pieces = {(0, 0): [own_a, own_b]}
    x_a, y_b = cross_x(own_a), cross_y(own_b)
    pieces[1, 0] = [x_a, cross_x(own_b)]
    if ny > 1:
        pieces[0, 1] = [cross_y(own_a), y_b]
        pieces[1, 1] = [cross_y(x_a), cross_x(y_b)]

    def row_weights(dx, dy):
        rows = []
        for step in range(nz):
            source = (((iz - step) % nz) * nx + (ix + dx) % nx) * ny + (iy + dy) % ny
            rows.append(lax.dynamic_index_in_dim(tables, source, axis=0, keepdims=False))
        rows = jnp.stack(rows)
        return jnp.concatenate([rows[:, :half].reshape(-1), rows[:, half:].reshape(-1)])[:, None]

    def expert(rows, scale):
        total = None
        for gate, up, down in (weights, peer_weights):
            gate_pre = jnp.dot(rows, gate, preferred_element_type=jnp.float32)
            up_pre = jnp.dot(rows, up, preferred_element_type=jnp.float32)
            gated = jnp.minimum(gate_pre, 7.0)
            upper = jnp.clip(up_pre, -7.0, 7.0)
            hidden = ((upper + 1.0) * gated * jax.nn.sigmoid(1.702 * gated)).astype(jnp.bfloat16)
            terms = jnp.dot(hidden, down, preferred_element_type=jnp.float32)
            total = terms if total is None else total + terms
        return (total * scale).astype(jnp.bfloat16)

    count = own_a.shape[0]
    parts = {}
    for place, rows in pieces.items():
        out = expert(jnp.concatenate(rows, axis=0), row_weights(*place))
        parts[place] = [out[:count], out[count:]]

    def added(*terms):
        total = terms[0].astype(jnp.float32)
        for term in terms[1:]:
            total = total + term.astype(jnp.float32)
        return total.astype(jnp.bfloat16)

    if ny > 1:
        y_a = cross_y(parts[0, 1][0])
        x_b = cross_x(parts[1, 0][1])
        x_a = cross_x(added(parts[1, 0][0], cross_y(parts[1, 1][0])))
        y_b = cross_y(added(parts[0, 1][1], cross_x(parts[1, 1][1])))
        sum_a = added(parts[0, 0][0], y_a, x_a)
        sum_b = added(parts[0, 0][1], x_b, y_b)
    else:
        sum_a = added(parts[0, 0][0], cross_x(parts[1, 0][0]))
        sum_b = added(parts[0, 0][1], cross_x(parts[1, 0][1]))

    def z_block(step):
        place = slice(step * half, (step + 1) * half)
        return jnp.concatenate([sum_a[place], sum_b[place]], axis=0)

    total = z_block(0).astype(jnp.float32)
    for step in range(1, nz):
        total = total + shift(z_block(step), "sz", -step).astype(jnp.float32)
    return total


def body(
    dense,
    residual,
    queries,
    keys,
    values,
    documents,
    sink,
    out_weight,
    mix_gain,
    ffn_gain,
    out_gain,
    routes,
    route_logits,
    gate_weight,
    up_weight,
    down_weight,
):
    tok_rows = queries.shape[0]
    head_count = queries.shape[1] // HD
    kv_count = keys.shape[1] // HD
    group_size = head_count // kv_count
    sp = ("sz", "sx") if dense else "sp"
    tp = ("ty", "tc") if dense else "tp"
    sp_count = lax.axis_size(sp)
    tp_count = lax.axis_size(tp)
    offset = lax.axis_index(sp) * tok_rows
    positions = offset + jnp.arange(tok_rows, dtype=jnp.int32)
    q_turned = turn_heads(queries, positions, head_count)
    k_turned = turn_heads(keys, positions, kv_count)
    paired = jnp.concatenate([k_turned, values], axis=1)
    wide_pairs, wide_docs = (
        extended(paired, ((sp, 0),), W),
        extended(documents, ((sp, 0),), W),
    )
    blocks = tok_rows // W
    query_blocks = q_turned.reshape(blocks, W, kv_count, group_size, HD)
    pair_win = windows(wide_pairs, blocks)
    key_win = pair_win[..., : kv_count * HD].reshape(blocks, 3 * W, kv_count, HD)
    value_win = pair_win[..., kv_count * HD :].reshape(blocks, 3 * W, kv_count, HD)
    doc_win = windows(wide_docs, blocks)
    doc_query = documents.reshape(blocks, W)
    block_ids = jnp.arange(blocks, dtype=jnp.int32)[:, None, None]
    query_pos = offset + block_ids * W + jnp.arange(W, dtype=jnp.int32)[None, :, None]
    key_pos = offset + (block_ids - 1) * W + jnp.arange(3 * W, dtype=jnp.int32)[None, None, :]
    keep_mask = (
        (jnp.abs(query_pos - key_pos) <= W) & (key_pos >= 0) & (key_pos < tok_rows * sp_count)
    )
    keep_mask = keep_mask & (doc_query[:, :, None] == doc_win[:, None, :])
    scores = jnp.einsum(
        "nqhgd,nkhd->nhgqk", query_blocks, key_win, preferred_element_type=jnp.float32
    ) * HD ** (-0.5)
    exponent = jnp.where(keep_mask[:, None, None], jnp.exp(scores), 0.0)
    denominator = jnp.sum(exponent, axis=-1, keepdims=True) + jnp.exp(sink).reshape(
        1, kv_count, group_size, 1, 1
    )
    probs = (exponent / denominator).astype(jnp.bfloat16)
    attended = jnp.einsum("nhgqk,nkhd->nqhgd", probs, value_win, preferred_element_type=jnp.float32)
    attended = attended.astype(jnp.bfloat16).reshape(tok_rows, head_count * HD)
    own_rows = tok_rows // tp_count
    all_heads = lax.all_to_all(attended, tp, split_axis=0, concat_axis=1, tiled=True)
    projected = jnp.dot(all_heads, out_weight, preferred_element_type=jnp.float32)
    after_mix = residual.astype(jnp.float32) + rms_scale(projected) * mix_gain
    normed = (rms_scale(after_mix) * ffn_gain).astype(jnp.bfloat16)
    exp_logits = jnp.exp(route_logits)
    route_weights = exp_logits / jnp.sum(exp_logits, axis=-1, keepdims=True)
    if dense and gate_weight.shape[0] == 1 and own_rows % 2 == 0:
        weights = (gate_weight[0], up_weight[0], down_weight[0])
        peer_weights = tuple(shift(weight, "tc", 1) for weight in weights)
        expert_mix = dense_experts(normed, routes, route_weights, weights, peer_weights)
    else:
        expert_mix = routed_experts(
            sp, tp, normed, routes, route_weights, gate_weight, up_weight, down_weight
        )
    return (after_mix + rms_scale(expert_mix) * out_gain).astype(jnp.bfloat16)


def solution(mesh):
    sp_count, tp_count = mesh.shape["sp"], mesh.shape["tp"]
    sp, tp = "sp", "tp"
    dense = sp_count <= 2 * TOPK and sp_count % 2 == 0 and tp_count % 2 == 0
    if dense:
        shape = (sp_count // 2, 2, tp_count // 2, 2)
        mesh = Mesh(mesh.devices.reshape(shape), ("sz", "sx", "ty", "tc"))
        sp, tp = ("sz", "sx"), ("ty", "tc")
    both = (sp if dense else (sp,)) + (tp if dense else (tp,))
    in_specs = (
        P(both, None),
        P(sp, tp),
        P(sp, tp),
        P(sp, tp),
        P(sp),
        P(tp),
        P(),
        P(),
        P(),
        P(),
        P(both, None),
        P(both, None),
        P(sp, None, tp),
        P(sp, None, tp),
        P(sp, tp, None),
    )
    return jax.shard_map(
        functools.partial(body, dense),
        mesh=mesh,
        in_specs=in_specs,
        out_specs=P(both, None),
        check_vma=False,
    )
```
